32 devices in a mesh: sp: 4 (over z), tp: 8 (over y, x, core).
Axes of the slice: x: 2, y: 2, z: 4, core: 2. Of those that a mesh axis runs over, the one named last changes fastest.
Arguments:
- tokens: bfloat16 [1536, 2048], P('sp', 'tp'), may hold values from -6 to 6
- norm_gain: bfloat16 [2048], replicated, may hold values from 0.099609375 to 1.8984375
- lin_query: bfloat16 [2048, 1024], P(None, 'tp'), may hold values from -0.125 to 0.125
- lin_key: bfloat16 [2048, 1024], P(None, 'tp'), may hold values from -0.125 to 0.125
- lin_value: bfloat16 [2048, 1024], P(None, 'tp'), may hold values from -0.125 to 0.125
- lin_gate: bfloat16 [2048, 1024], P(None, 'tp'), may hold values from -0.125 to 0.125
- gate_down: bfloat16 [2048, 32], replicated, may hold values from -0.125 to 0.125
- gate_up_weight: bfloat16 [32, 1024], replicated, may hold values from -1 to 1
- decay_offset_bias: float32 [1536, 1024], P('sp', 'tp'), may hold values from -16 to 11
- lin_norm_gain: float32 [128], replicated, may hold values from 0.1 to 1.9
- stick_query: bfloat16 [2048, 1024], P(None, 'tp'), may hold values from -0.25 to 0.25
- stick_key: bfloat16 [2048, 1024], P(None, 'tp'), may hold values from -0.25 to 0.25
- stick_value: bfloat16 [2048, 1024], P(None, 'tp'), may hold values from -0.125 to 0.125
- key_bias: bfloat16 [8, 1536], P('tp', 'sp'), may hold values from -20 to -2
- out_linear: bfloat16 [1024, 2048], replicated, may hold values from -0.125 to 0.125
- out_stick: bfloat16 [1024, 2048], replicated, may hold values from -0.125 to 0.125
Outputs:
- mixed: bfloat16 [1536, 2048], P(('sp', 'tp'))
The draws below stay inside these ranges and needn't reach their ends.
All inputs are finite; a program needn't handle non-finite values.
Results may differ from the reference program's by a relative error of at most 0.012.
Values may be sent and summed in bfloat16 or wider, within the bound.
A program may use at most 64 MiB of HBM per device.

```python
import math
import jax
import jax.numpy as jnp
from jax import lax

D = 2048
GH = 8
HS = 8
DK = 128
RANK = 32
BLK = 32
TOK_DEV = 384
SEQUENCE_LENGTH = 1536


def segment_rows(key_segment):
    position_index = jax.random.randint(key_segment, (4,), 0, SEQUENCE_LENGTH)
    return jnp.any(jnp.arange(SEQUENCE_LENGTH)[:, None] == position_index[None, :], axis=1)


def draw_decay_offset_bias(key, part):
    key_rows = jax.random.split(jax.random.fold_in(key, 11), 5)
    slow_heads = jax.random.randint(key_rows[0], (GH,), 0, 2) > 0
    span_count = SEQUENCE_LENGTH // TOK_DEV
    offsets = jax.random.uniform(key_rows[1], (span_count, GH), jnp.float32, -0.7, 0.7)
    span_of = jnp.arange(SEQUENCE_LENGTH) // TOK_DEV
    fast_level = jax.random.uniform(key_rows[2], (GH,), jnp.float32, -0.5, 1.5)
    level = jnp.where(slow_heads, 9.5, fast_level)
    head_wise = level[None, :] + offsets[span_of]
    random_jitter = jax.random.uniform(key_rows[3], (SEQUENCE_LENGTH, GH, DK), jnp.float32, -0.5, 0.5)
    segment_list = segment_rows(key_rows[4]).astype(jnp.float32)
    value_rows = head_wise[:, :, None] + random_jitter - 14.0 * segment_list[:, None, None]
    return value_rows.reshape(SEQUENCE_LENGTH, GH * DK)


def draw_key_bias(key, part):
    key_rows = jax.random.split(jax.random.fold_in(key, 23), 5)
    slow_heads = jax.random.randint(key_rows[0], (HS,), 0, 2) > 0
    span_count = SEQUENCE_LENGTH // TOK_DEV
    offsets = jax.random.uniform(key_rows[1], (HS, span_count), jnp.float32, -0.7, 0.7)
    span_of = jnp.arange(SEQUENCE_LENGTH) // TOK_DEV
    fast_level = jax.random.uniform(key_rows[2], (HS,), jnp.float32, -12.5, -11.5)
    level = jnp.where(slow_heads, -8.0 - math.log(SEQUENCE_LENGTH), fast_level)
    head_wise = level[:, None] + offsets[:, span_of]
    random_jitter = jax.random.uniform(key_rows[3], (HS, SEQUENCE_LENGTH), jnp.float32, -0.5, 0.5)
    segment_list = segment_rows(key_rows[4]).astype(jnp.float32)
    value_rows = head_wise + random_jitter + 8.0 * segment_list[None, :]
    return value_rows.astype(jnp.bfloat16)


def shard_levels(rng, extent, pieces, low, largest):
    factor_of = 1.0
    for axis_at, blocks in pieces:
        draws = jax.random.uniform(jax.random.fold_in(jax.random.fold_in(rng, 6), axis_at), (blocks,), jnp.float32, low / len(pieces), largest / len(pieces))
        factor_of = factor_of * jnp.repeat(jnp.exp(draws), extent[axis_at] // blocks).reshape((-1,) + (1,) * (len(extent) - 1 - axis_at))
    return factor_of


def noise(stream_key, shape, scale, bound, pieces=(), held_as=jnp.bfloat16):
    factor_of = shard_levels(stream_key, shape, pieces, -0.22, 0.18) if pieces else 1.0
    values = jax.random.normal(stream_key, shape, jnp.float32) * scale * factor_of
    return jnp.minimum(jnp.maximum(values, -bound), bound).astype(held_as)


def setup_inputs(seed: int = 0) -> dict:
    splits = jax.random.split(jax.random.key(seed), 17)
    tokens = noise(splits[0], (SEQUENCE_LENGTH, D), 1.0, 6.0, ((0, 4), (1, 8)))
    norm_gain = jnp.clip(1.0 + 0.18 * jax.random.normal(splits[1], (D,), jnp.float32), 0.099609375, 1.8984375).astype(jnp.bfloat16)
    lin_query = noise(splits[2], (D, GH * DK), D ** -0.5, 0.125, ((1, 8),))
    lin_key = noise(splits[3], (D, GH * DK), D ** -0.5, 0.125, ((1, 8),))
    lin_value = noise(splits[4], (D, GH * DK), D ** -0.5, 0.125, ((1, 8),))
    lin_gate = noise(splits[5], (D, GH * DK), D ** -0.5, 0.125, ((1, 8),))
    gate_down = noise(splits[6], (D, RANK), D ** -0.5, 0.125)
    gate_up_weight = noise(splits[7], (RANK, GH * DK), RANK ** -0.5, 1.0)
    decay_offset_bias = draw_decay_offset_bias(jax.random.fold_in(splits[16], 71), 0)
    lin_norm_gain = jnp.clip(1.0 + 0.18 * jax.random.normal(splits[9], (DK,), jnp.float32), 0.1, 1.9)
    stick_query = noise(splits[10], (D, HS * DK), (D // 4) ** -0.5, 0.25, ((1, 8),))
    stick_key = noise(splits[11], (D, HS * DK), (D // 4) ** -0.5, 0.25, ((1, 8),))
    stick_value = noise(splits[12], (D, HS * DK), D ** -0.5, 0.125, ((1, 8),))
    key_bias = draw_key_bias(jax.random.fold_in(splits[16], 71), 0)
    out_linear = noise(splits[14], (GH * DK, D), (GH * DK + HS * DK) ** -0.5, 0.125)
    out_stick = noise(splits[15], (HS * DK, D), (GH * DK + HS * DK) ** -0.5, 0.125)
    return {"tokens": tokens, "norm_gain": norm_gain, "lin_query": lin_query, "lin_key": lin_key, "lin_value": lin_value, "lin_gate": lin_gate, "gate_down": gate_down, "gate_up_weight": gate_up_weight, "decay_offset_bias": decay_offset_bias, "lin_norm_gain": lin_norm_gain, "stick_query": stick_query, "stick_key": stick_key, "stick_value": stick_value, "key_bias": key_bias, "out_linear": out_linear, "out_stick": out_stick}


norm_eps = 1e-06
gate_softness = 16.0

def linear_attention(queries, keys_in, values_in, decay_logarithm, gate_in, head_gain):
    blocks = SEQUENCE_LENGTH // BLK
    highest_precision = lax.Precision.HIGHEST

    def blocked(matrix):
        return matrix.reshape(blocks, BLK, GH, DK).transpose(0, 2, 1, 3)
    causal = jnp.tril(jnp.ones((BLK, BLK), dtype=bool))

    def advance(running_state, inputs):
        query_block, key_block, value_block, decay_blk = inputs
        within_segment = jnp.cumsum(decay_blk, axis=1)
        carried_state = jnp.einsum('cgw,cwz->cgz', query_block * jnp.exp(within_segment), running_state, precision=highest_precision)
        spread = within_segment[:, :, None, :] - within_segment[:, None, :, :]
        fading = jnp.exp(jnp.where(causal[:, :, None], spread, -jnp.inf))
        scores = jnp.einsum('htk,hsk,htsk->hts', query_block, key_block, fading, precision=highest_precision)
        rounded = lax.optimization_barrier(scores.astype(jnp.bfloat16))
        inner = jnp.einsum('hts,hsv->htv', rounded.astype(jnp.float32), value_block.astype(jnp.float32), precision=highest_precision)
        last_position = within_segment[:, -1, :]
        fresh_state = jnp.einsum('iga,igl->ial', key_block * jnp.exp(last_position[:, None, :] - within_segment), value_block.astype(jnp.float32), precision=highest_precision)
        new_state = running_state * jnp.exp(last_position)[:, :, None] + fresh_state
        return (new_state, carried_state + inner)
    scaled_queries = blocked(queries).astype(jnp.float32) * DK ** (-0.5)
    start_state = jnp.zeros((GH, DK, DK), jnp.float32)
    _, outputs = lax.scan(advance, start_state, (scaled_queries, blocked(keys_in).astype(jnp.float32), blocked(values_in), blocked(decay_logarithm)))
    combined = outputs.transpose(0, 2, 1, 3).reshape(SEQUENCE_LENGTH, GH, DK)
    normed = combined * lax.rsqrt(lax.optimization_barrier(jnp.mean(combined * combined, axis=-1, keepdims=True)) + norm_eps) * head_gain
    return (normed.reshape(SEQUENCE_LENGTH, GH * DK) * jax.nn.silu(gate_in.astype(jnp.float32))).astype(jnp.bfloat16)

def stick_attention(queries, keys_in, values_in, key_bias):
    span_count = SEQUENCE_LENGTH // TOK_DEV
    key_pos = jnp.arange(SEQUENCE_LENGTH, dtype=jnp.int32)

    def head_wise(matrix):
        return matrix.reshape(SEQUENCE_LENGTH, HS, DK).transpose(1, 0, 2)

    def one_head(inputs):
        head_query, head_key, head_value, head_bias = inputs
        starts = jnp.arange(span_count, dtype=jnp.int32) * TOK_DEV

        def one_span(span_in):
            span_query, first = span_in
            logits = jnp.dot(span_query, head_key.T, preferred_element_type=jnp.float32) * DK ** (-0.5) + head_bias.astype(jnp.float32)[None, :]
            query_pos = first + jnp.arange(TOK_DEV, dtype=jnp.int32)
            visible = key_pos[None, :] < query_pos[:, None]
            falling = jnp.where(visible, jax.nn.log_sigmoid(-logits), 0.0)
            behind = lax.cumsum(falling, axis=1, reverse=True) - falling
            shares = jnp.where(visible, jnp.exp(jax.nn.log_sigmoid(logits) + behind), 0.0).astype(jnp.bfloat16)
            return jnp.dot(shares, head_value, preferred_element_type=jnp.float32)
        spans = lax.map(one_span, (head_query.reshape(span_count, TOK_DEV, DK), starts))
        return spans.reshape(SEQUENCE_LENGTH, DK)
    heads_out = lax.map(one_head, (head_wise(queries), head_wise(keys_in), head_wise(values_in), key_bias))
    return heads_out.transpose(1, 0, 2).reshape(SEQUENCE_LENGTH, HS * DK).astype(jnp.bfloat16)

def reference(tokens, norm_gain, lin_query, lin_key, lin_value, lin_gate, gate_down, gate_up_weight, decay_offset_bias, lin_norm_gain, stick_query, stick_key, stick_value, key_bias, out_linear, out_stick):
    widened = tokens.astype(jnp.float32)
    inv_rms = lax.rsqrt(lax.optimization_barrier(jnp.mean(widened * widened, axis=1)) + norm_eps)[:, None]
    scaled = (widened * norm_gain.astype(jnp.float32)).astype(jnp.bfloat16)

    def project(weight):
        return (jnp.dot(scaled, weight, preferred_element_type=jnp.float32) * inv_rms).astype(jnp.bfloat16)
    reduced_rank = project(gate_down)
    decay_logarithm = jax.nn.log_sigmoid(jnp.dot(reduced_rank, gate_up_weight, preferred_element_type=jnp.float32) + decay_offset_bias) / gate_softness
    linear_out = linear_attention(project(lin_query), project(lin_key), project(lin_value), decay_logarithm, project(lin_gate), lin_norm_gain)
    stick_out = stick_attention(project(stick_query), project(stick_key), project(stick_value), key_bias)
    total = jnp.dot(linear_out, out_linear, preferred_element_type=jnp.float32) + jnp.dot(stick_out, out_stick, preferred_element_type=jnp.float32)
    return total.astype(jnp.bfloat16)
```

```python
import functools
import jax
import jax.numpy as jnp
from jax import lax
from jax.experimental import pallas as pl
from jax.experimental.pallas import tpu as pltpu
from jax.sharding import PartitionSpec as P

norm_eps = 1e-06
gate_softness = 16.0
CHUNK = 128
F32 = jnp.float32
BF16 = jnp.bfloat16
NT = (((1,), (1,)), ((), ()))
TN = (((0,), (0,)), ((), ()))


def fdot(a, b):
    return jnp.dot(a, b, preferred_element_type=F32)


def gdot(a, b, dims):
    return lax.dot_general(a, b, dims, preferred_element_type=F32)


def kernel(
    n_sp,
    n_tp,
    tokens,
    gain,
    lq_w,
    lk_w,
    lv_w,
    lg_w,
    sq_w,
    sk_w,
    sv_w,
    gd_w,
    gu_w,
    dbias,
    head_gain,
    kbias,
    ol_w,
    os_w,
    out,
    w_s,
    gd_s,
    gu_s,
    db_s,
    wol,
    wos,
    tok,
    acc,
    acc_low,
    squares,
    lin_b,
    dlog,
    qx,
    kv,
    bias_s,
    tri,
    o_acc,
    cons,
    far_o,
    far_c,
    far_out,
    ret,
    fin,
    local,
    qstart,
    st_buf,
    td_buf,
    lin_o,
    stk_o,
    lin_r,
    stk_r,
    wsem,
    tok_send,
    tok_recv,
    q_send,
    q_recv,
    ret_send,
    ret_recv,
    bias_send,
    bias_recv,
    kv_send,
    kv_recv,
    st_send,
    st_recv,
    td_send,
    td_recv,
    al_send,
    al_recv,
    as_send,
    as_recv,
):
    me = lax.axis_index("tp")
    here = lax.axis_index("sp")
    T, F = tokens.shape
    H = T // 2
    DK = lq_w.shape[1]
    D = lq_w.shape[0]
    rows_out = T // n_tp
    scale = DK ** (-0.5)
    balanced = n_sp == 4
    reach = 2 if balanced else n_sp

    copies = []
    for i, w in enumerate((sk_w, sv_w, sq_w, lq_w, lk_w, lv_w, lg_w)):
        copies.append(pltpu.make_async_copy(w, w_s.at[:, pl.ds(i * DK, DK)], wsem.at[i]))
    copies.append(pltpu.make_async_copy(gd_w, gd_s, wsem.at[7]))
    col = pl.multiple_of(me * DK, DK)
    copies.append(pltpu.make_async_copy(gu_w.at[:, pl.ds(col, DK)], gu_s, wsem.at[8]))
    copies.append(pltpu.make_async_copy(dbias, db_s, wsem.at[9]))
    copies.append(pltpu.make_async_copy(ol_w, wol, wsem.at[10]))
    copies.append(pltpu.make_async_copy(os_w, wos, wsem.at[11]))
    for c in copies:
        c.start()

    barrier = pltpu.get_barrier_semaphore()
    for d in range(1, n_tp):
        pl.semaphore_signal(
            barrier, inc=1, device_id={"tp": (me + d) % n_tp}, device_id_type=pl.DeviceIdType.MESH
        )
    for d in range(1, n_sp):
        pl.semaphore_signal(
            barrier, inc=1, device_id={"sp": (here + d) % n_sp}, device_id_type=pl.DeviceIdType.MESH
        )
    pl.semaphore_wait(barrier, n_tp + n_sp - 2)

    def remote(src, dst, send, recv, where):
        return pltpu.make_async_remote_copy(
            src_ref=src,
            dst_ref=dst,
            send_sem=send,
            recv_sem=recv,
            device_id=where,
            device_id_type=pl.DeviceIdType.MESH,
        )

    core = me % 2
    chip = me // 2
    side = 1 - 2 * core
    partner = me + side
    x_chip = chip + 1 - 2 * (chip % 2)
    y_step = 2 * (1 - 2 * (chip // 2))
    y_chip = chip + y_step
    d_chip = x_chip + y_step
    x_dev, y_dev, d_dev = 2 * x_chip + core, 2 * y_chip + core, 2 * d_chip + core

    sent = []

    def piece(ref, h):
        return ref.at[pl.ds(h * H, H)]

    def send_tok(src, h, target, own=False):
        dst = tok.at[src, pl.ds(h * H, H)]
        c = remote(
            piece(tokens, h) if own else dst,
            dst,
            tok_send.at[len(sent)],
            tok_recv.at[src, h],
            {"tp": target},
        )
        c.start()
        sent.append(c)

    def wait_tok(src, h):
        dst = tok.at[src, pl.ds(h * H, H)]
        remote(dst, dst, tok_send.at[0], tok_recv.at[src, h], {"tp": partner}).wait_recv()

    send_tok(me, 0, x_dev, True)
    send_tok(me, 1, y_dev, True)
    send_tok(me, 1, x_dev, True)
    send_tok(me, 0, y_dev, True)
    send_tok(me, 0, partner, True)
    send_tok(me, 1, partner, True)

    bias_s[here] = jnp.broadcast_to(kbias[...].astype(F32), bias_s.shape[1:])

    def later(d, make):
        @pl.when(here + d < n_sp)
        def _():
            make(d)

    def bias_copy(d):
        return remote(
            bias_s.at[here], bias_s.at[here], bias_send.at[d], bias_recv.at[here], {"sp": here + d}
        )

    for d in range(1, reach):
        later(d, lambda d: bias_copy(d).start())

    rr = lax.broadcasted_iota(jnp.int32, (T, T), 0)
    cc = lax.broadcasted_iota(jnp.int32, (T, T), 1)
    tri[...] = jnp.where(rr > cc, 1.0, 0.0).astype(BF16)

    def project(src, ref, first=False):
        at = pl.ds(pl.multiple_of(src * F, F), F)
        raw = ref[...].astype(F32)
        sq = raw * raw
        part = sq[:, :128]
        for i in range(1, F // 128):
            part = part + sq[:, i * 128 : (i + 1) * 128]
        scaled = (raw * gain[at].astype(F32)[None, :]).astype(BF16)
        main = fdot(scaled, w_s[at, :])
        low = gdot(scaled, gd_s[:, at], NT)
        if first:
            squares[...] = part
            acc[...] = main
            acc_low[...] = low
        else:
            squares[...] += part
            acc[...] += main
            acc_low[...] += low

    for i in range(8):
        copies[i].wait()
    project(me, tokens, True)
    wait_tok(partner, 0)
    wait_tok(partner, 1)
    project(partner, tok.at[partner])
    wait_tok(x_dev, 0)
    send_tok(x_dev, 0, y_dev)
    send_tok(x_dev, 0, partner)
    wait_tok(y_dev, 1)
    send_tok(y_dev, 1, x_dev)
    send_tok(y_dev, 1, partner)
    wait_tok(x_dev, 1)
    send_tok(x_dev, 1, partner)
    wait_tok(y_dev, 0)
    send_tok(y_dev, 0, partner)
    project(x_dev, tok.at[x_dev])
    project(y_dev, tok.at[y_dev])
    for p in (x_dev + side, y_dev + side):
        wait_tok(p, 0)
        wait_tok(p, 1)
        project(p, tok.at[p])
    wait_tok(d_dev, 0)
    send_tok(d_dev, 0, partner)
    wait_tok(d_dev, 1)
    send_tok(d_dev, 1, partner)
    project(d_dev, tok.at[d_dev])
    wait_tok(d_dev + side, 0)
    wait_tok(d_dev + side, 1)
    project(d_dev + side, tok.at[d_dev + side])

    inv = lax.rsqrt(jnp.sum(squares[...], axis=1, keepdims=True) / D + norm_eps)

    def proj(i):
        return (acc[:, i * DK : (i + 1) * DK] * inv).astype(BF16)

    kv[here, 0] = proj(0)
    kv[here, 1] = proj(1)

    C = CHUNK

    def kv_copy(j, s):
        return remote(kv.at[j], kv.at[j], kv_send.at[s], kv_recv.at[j], {"sp": here + 1})

    split = 0
    parts = ((split, T), (0, split)) if split else ((0, T),)

    def kv_part(j, i):
        lo, hi = parts[i]
        view = kv.at[j, :, pl.ds(lo, hi - lo)]
        return remote(view, view, kv_send.at[i], kv_recv.at[i], {"sp": here + 1})

    @pl.when(here + 1 < n_sp)
    def _():
        if balanced:
            for i in range(len(parts)):
                kv_part(here, i).start()
        else:
            kv_copy(here, 0).start()

    qx[0] = proj(2)

    def q_copy(slot):
        return remote(qx.at[0], qx.at[slot], q_send.at[slot], q_recv.at[slot], {"sp": 2 - slot})

    def ret_copy(i, r, target):
        at = pl.ds(r * C, C)
        return remote(
            far_out.at[i, at], ret.at[at], ret_send.at[i, r], ret_recv.at[r], {"sp": target}
        )

    if balanced:

        @pl.when(here == 3)
        def _():
            q_copy(1).start()

        @pl.when(here == 2)
        def _():
            q_copy(2).start()

    for i in range(4):
        lin_b[i] = proj(3 + i)
    for i in range(8, 10):
        copies[i].wait()
    low = (acc_low[...] * inv).astype(BF16)
    pre = fdot(low, gu_s[...]) + db_s[...]
    dlog[...] = (
        jnp.minimum(pre, 0.0) - jnp.log(1.0 + jnp.exp(-jnp.abs(pre)))
    ) / gate_softness

    row = lax.broadcasted_iota(jnp.int32, (C, DK), 0)
    rc = lax.broadcasted_iota(jnp.int32, (C, C), 0)
    ccol = lax.broadcasted_iota(jnp.int32, (C, C), 1)
    tri_c = jnp.where(rc >= ccol, 1.0, 0.0).astype(F32)

    def chunk(n, carry):
        state, offset = carry
        at = pl.ds(pl.multiple_of(n * C, C), C)
        lam = dlog[at, :]
        c = jnp.dot(tri_c, lam, preferred_element_type=F32, precision=lax.Precision.HIGHEST)
        q = lin_b[0, at, :].astype(F32) * scale
        k = lin_b[1, at, :].astype(F32)
        v = lin_b[2, at, :]
        v32 = v.astype(F32)
        scores = jnp.zeros((C, C), F32)
        m = C // 2
        while m >= 8:
            grouped = c.reshape(C // (2 * m), 2 * m, DK)
            middle = jnp.broadcast_to(grouped[:, m - 1 : m, :], grouped.shape).reshape(C, DK)
            upper = row % (2 * m) >= m
            a = jnp.where(upper, q, k) * jnp.exp(jnp.where(upper, c - middle, middle - c))
            ab = a.astype(BF16)
            pair = gdot(ab, ab, NT)
            keep = (
                (rc // (2 * m) == ccol // (2 * m))
                & (rc % (2 * m) >= m)
                & (ccol % (2 * m) < m)
            )
            scores = jnp.where(keep, pair, scores)
            m //= 2
        total = fdot(scores.astype(BF16), v)
        for delta in range(8):
            if delta == 0:
                p = jnp.sum(q * k, axis=1, keepdims=True)
                total = total + p * v32
                continue
            kd = pltpu.roll(k, delta, 0)
            cd = pltpu.roll(c, delta, 0)
            vd = pltpu.roll(v32, delta, 0)
            p = jnp.sum(q * kd * jnp.exp(jnp.minimum(c - cd, 0.0)), axis=1, keepdims=True)
            total = total + jnp.where(row % 8 >= delta, p * vd, 0.0)
        total = total + gdot((q * jnp.exp(c)).astype(BF16), state.astype(BF16), NT)
        local[at, :] = total
        qstart[at, :] = (q * jnp.exp(offset + c)).astype(BF16)
        last = c[C - 1 : C, :]
        kk = (k * jnp.exp(last - c)).astype(BF16)
        state = state * jnp.exp(last) + gdot(v, kk, TN)
        return state, offset + last

    state, offset = lax.fori_loop(
        0, T // C, chunk, (jnp.zeros((DK, DK), F32), jnp.zeros((1, DK), F32))
    )
    st_buf[here] = state.astype(BF16)
    td_buf[here] = jnp.broadcast_to(offset, td_buf.shape[1:])

    def st_copy(d):
        return remote(
            st_buf.at[here], st_buf.at[here], st_send.at[d], st_recv.at[here], {"sp": here + d}
        )

    def td_copy(d):
        return remote(
            td_buf.at[here], td_buf.at[here], td_send.at[d], td_recv.at[here], {"sp": here + d}
        )

    for d in range(n_sp - 1, 0, -1):
        later(d, lambda d: st_copy(d).start())
        later(d, lambda d: td_copy(d).start())

    def stick(slot, j, mode, o_ref, c_ref, keys=(0, T), finish=None):
        own = mode == "own"
        lo = keys[0]
        for r in range(T // C):
            at = pl.ds(r * C, C)
            n = (r + 1) * C if own else keys[1] - lo
            bias = bias_s[j, 0:1, pl.ds(lo, n)]
            z = gdot(qx[slot, at, :], kv[j, 0, pl.ds(lo, n), :], NT) * scale + bias
            soft = jnp.log(1.0 + jnp.exp(-jnp.abs(z)))
            rise = jnp.minimum(z, 0.0) - soft
            fall = jnp.minimum(-z, 0.0) - soft
            if own:
                tr = lax.broadcasted_iota(jnp.int32, (C, n), 0) + r * C
                visible = lax.broadcasted_iota(jnp.int32, (C, n), 1) < tr
                fall = jnp.where(visible, fall, 0.0)
            high = fall.astype(BF16)
            rest = (fall - high.astype(F32)).astype(BF16)
            later_keys = tri[pl.ds(0, n), pl.ds(0, n)]
            behind = fdot(high, later_keys) + fdot(rest, later_keys)
            power = rise + behind
            if mode == "add":
                power = power + c_ref[at, 0:1]
            share = jnp.exp(power)
            if own:
                share = jnp.where(visible, share, 0.0)
            value = fdot(share.astype(BF16), kv[j, 1, pl.ds(lo, n), :])
            spent = jnp.broadcast_to(behind[:, 0:1] + fall[:, 0:1], (C, DK))
            if mode == "add":
                value = value + o_ref[at, :]
                spent = spent + c_ref[at, :]
            if finish is None:
                o_ref[at, :] = value
                c_ref[at, :] = spent
            else:
                finish(r, value)

    stick(0, here, "own", o_acc, cons)

    def await_kv(j, s):
        remote(kv.at[j], kv.at[j], kv_send.at[s], kv_recv.at[j], {"sp": here}).wait_recv()

    def await_bias(j):
        remote(
            bias_s.at[j], bias_s.at[j], bias_send.at[0], bias_recv.at[j], {"sp": here}
        ).wait_recv()

    def take(s):
        j = here - s
        await_kv(j, s)

        @pl.when(here + 1 < n_sp)
        def _():
            kv_copy(j, s).start()

        await_bias(j)
        stick(0, j, "add", o_acc, cons)

    def give(i, target):
        def finish(r, value):
            far_out[i, pl.ds(r * C, C), :] = value.astype(BF16)
            ret_copy(i, r, target).start()

        return finish

    if balanced:
        last = len(parts) - 1

        @pl.when(here == 1)
        def _():
            q_copy(1).wait_recv()
            stick(1, 1, "start", far_o, far_c)
            await_bias(0)
            for i in range(len(parts)):
                kv_part(0, i).wait_recv()
                stick(1, 0, "add", far_o, far_c, parts[i], give(0, 3) if i == last else None)

        @pl.when(here == 0)
        def _():
            q_copy(2).wait_recv()
            stick(2, 0, "start", far_o, far_c, finish=give(1, 2))

        @pl.when(here >= 2)
        def _():
            await_bias(here - 1)
            for i in range(len(parts)):
                kv_part(here - 1, i).wait_recv()
            stick(0, here - 1, "add", o_acc, cons)

    else:

        @pl.when(here >= 1)
        def _():
            take(1)

    def gather_state(j, incoming):
        remote(st_buf.at[j], st_buf.at[j], st_send.at[0], st_recv.at[j], {"sp": here}).wait_recv()
        remote(td_buf.at[j], td_buf.at[j], td_send.at[0], td_recv.at[j], {"sp": here}).wait_recv()
        return incoming * jnp.exp(td_buf[j][0:1, :]) + st_buf[j].astype(F32)

    incoming = lax.fori_loop(0, here, gather_state, jnp.zeros((DK, DK), F32))
    combined = local[...] + gdot(qstart[...], incoming.astype(BF16), NT)
    normed = (
        combined
        * lax.rsqrt(jnp.mean(combined * combined, axis=1, keepdims=True) + norm_eps)
        * head_gain[...]
    )
    gate = lin_b[3].astype(F32)
    lin_o[...] = (normed * (gate / (1.0 + jnp.exp(-gate)))).astype(BF16)

    def exchange(source, landing, send, recv):
        done = []
        for d in range(1, n_tp):
            p = (me + d) % n_tp
            c = remote(
                source.at[pl.ds(pl.multiple_of(p * rows_out, rows_out), rows_out)],
                landing.at[me],
                send.at[d],
                recv.at[me],
                {"tp": p},
            )
            c.start()
            done.append(c)
        own = pl.ds(pl.multiple_of(me * rows_out, rows_out), rows_out)
        landing[me] = source[own, :]
        return done

    def arrive(landing, recv):
        for d in range(1, n_tp):
            p = (me + d) % n_tp
            remote(landing.at[p], landing.at[p], recv.at[p], recv.at[p], {"tp": p}).wait_recv()

    lin_sent = exchange(lin_o, lin_r, al_send, al_recv)

    if balanced:

        @pl.when(here == 1)
        def _():
            stick(0, 0, "add", o_acc, cons)

        @pl.when(here >= 2)
        def _():
            for r in range(T // C):
                ret_copy(0, r, here).wait_recv()
            o_acc[...] += jnp.exp(cons[...]) * ret[...].astype(F32)

    else:

        def more(s, carry):
            take(s)
            return carry

        lax.fori_loop(2, here + 1, more, 0)

    stk_o[...] = o_acc[...].astype(BF16)
    stk_sent = exchange(stk_o, stk_r, as_send, as_recv)
    copies[10].wait()
    copies[11].wait()
    arrive(lin_r, al_recv)

    def gathered(landing):
        return jnp.concatenate([landing[p] for p in range(n_tp)], axis=1)

    fin[...] = fdot(gathered(lin_r), wol[...])
    arrive(stk_r, as_recv)
    out[...] = (fin[...] + fdot(gathered(stk_r), wos[...])).astype(BF16)

    for c in sent + lin_sent + stk_sent:
        c.wait_send()
    for d in range(1, reach):
        later(d, lambda d: bias_copy(d).wait_send())
    for d in range(1, n_sp):
        later(d, lambda d: st_copy(d).wait_send())
        later(d, lambda d: td_copy(d).wait_send())

    @pl.when(here + 1 < n_sp)
    def _():
        if balanced:
            for i in range(len(parts)):
                kv_part(here, i).wait_send()
        else:

            def drain(s, carry):
                kv_copy(here - s, s).wait_send()
                return carry

            lax.fori_loop(0, here + 1, drain, 0)

    if balanced:

        @pl.when(here == 3)
        def _():
            q_copy(1).wait_send()

        @pl.when(here == 2)
        def _():
            q_copy(2).wait_send()

        @pl.when(here == 1)
        def _():
            for r in range(T // C):
                ret_copy(0, r, 3).wait_send()

        @pl.when(here == 0)
        def _():
            for r in range(T // C):
                ret_copy(1, r, 2).wait_send()


def per_device(n_sp, n_tp, *args):
    (
        tokens,
        norm_gain,
        lin_query,
        lin_key,
        lin_value,
        lin_gate,
        gate_down,
        gate_up_weight,
        decay_offset_bias,
        lin_norm_gain,
        stick_query,
        stick_key,
        stick_value,
        key_bias,
        out_linear,
        out_stick,
    ) = args
    T, F = tokens.shape
    D, DK = lin_query.shape
    rank = gate_down.shape[1]
    rows_out = T // n_tp
    width = out_linear.shape[1]
    vm = pl.BlockSpec(memory_space=pltpu.VMEM)
    anywhere = pl.BlockSpec(memory_space=pl.ANY)
    dma = pltpu.SemaphoreType.DMA
    return pl.pallas_call(
        functools.partial(kernel, n_sp, n_tp),
        out_shape=pltpu.VMEM((rows_out, width), BF16),
        in_specs=[vm, vm] + [anywhere] * 10 + [vm, vm, anywhere, anywhere],
        out_specs=vm,
        scratch_shapes=[
            pltpu.VMEM((D, 7 * DK), BF16),
            pltpu.VMEM((rank, D), BF16),
            pltpu.VMEM((rank, DK), BF16),
            pltpu.VMEM((T, DK), F32),
            pltpu.VMEM(out_linear.shape, BF16),
            pltpu.VMEM(out_stick.shape, BF16),
            pltpu.VMEM((n_tp, T, F), BF16),
            pltpu.VMEM((T, 7 * DK), F32),
            pltpu.VMEM((T, rank), F32),
            pltpu.VMEM((T, 128), F32),
            pltpu.VMEM((4, T, DK), BF16),
            pltpu.VMEM((T, DK), F32),
            pltpu.VMEM((3, T, DK), BF16),
            pltpu.VMEM((n_sp, 2, T, DK), BF16),
            pltpu.VMEM((n_sp, 8, T), F32),
            pltpu.VMEM((T, T), BF16),
            pltpu.VMEM((T, DK), F32),
            pltpu.VMEM((T, DK), F32),
            pltpu.VMEM((T, DK), F32),
            pltpu.VMEM((T, DK), F32),
            pltpu.VMEM((2, T, DK), BF16),
            pltpu.VMEM((T, DK), BF16),
            pltpu.VMEM((rows_out, width), F32),
            pltpu.VMEM((T, DK), F32),
            pltpu.VMEM((T, DK), BF16),
            pltpu.VMEM((n_sp, DK, DK), BF16),
            pltpu.VMEM((n_sp, 8, DK), F32),
            pltpu.VMEM((T, DK), BF16),
            pltpu.VMEM((T, DK), BF16),
            pltpu.VMEM((n_tp, rows_out, DK), BF16),
            pltpu.VMEM((n_tp, rows_out, DK), BF16),
            dma((12,)),
            dma((16,)),
            dma((n_tp, 2)),
            dma((3,)),
            dma((3,)),
            dma((2, T // CHUNK)),
            dma((T // CHUNK,)),
            dma((n_sp,)),
            dma((n_sp,)),
            dma((n_sp,)),
            dma((n_sp,)),
            dma((n_sp,)),
            dma((n_sp,)),
            dma((n_sp,)),
            dma((n_sp,)),
            dma((n_tp,)),
            dma((n_tp,)),
            dma((n_tp,)),
            dma((n_tp,)),
        ],
        compiler_params=pltpu.CompilerParams(collective_id=0, has_side_effects=True),
    )(
        tokens,
        norm_gain,
        lin_query,
        lin_key,
        lin_value,
        lin_gate,
        stick_query,
        stick_key,
        stick_value,
        gate_down.T,
        gate_up_weight,
        decay_offset_bias,
        lin_norm_gain.reshape(1, DK),
        key_bias,
        out_linear,
        out_stick,
    )


def solution(mesh):
    placed = (
        P("sp", "tp"),
        P(),
        P(None, "tp"),
        P(None, "tp"),
        P(None, "tp"),
        P(None, "tp"),
        P(),
        P(),
        P("sp", "tp"),
        P(),
        P(None, "tp"),
        P(None, "tp"),
        P(None, "tp"),
        P("tp", "sp"),
        P(),
        P(),
    )
    return jax.shard_map(
        functools.partial(per_device, mesh.shape["sp"], mesh.shape["tp"]),
        mesh=mesh,
        in_specs=placed,
        out_specs=P(("sp", "tp"), None),
        check_vma=False,
    )
```

```python
import functools
import jax
import jax.numpy as jnp
from jax import lax
from jax.experimental import pallas as pl
from jax.experimental.pallas import tpu as pltpu
from jax.sharding import PartitionSpec as P

norm_eps = 1e-06
gate_softness = 16.0
CHUNK = 128
LOG2E = 1.4426950408889634
F32 = jnp.float32
BF16 = jnp.bfloat16
NT = (((1,), (1,)), ((), ()))
TN = (((0,), (0,)), ((), ()))


def fdot(a, b):
    return jnp.dot(a, b, preferred_element_type=F32)


def gdot(a, b, dims):
    return lax.dot_general(a, b, dims, preferred_element_type=F32)


def kernel(
    n_sp,
    n_tp,
    tokens,
    gain,
    lq_w,
    lk_w,
    lv_w,
    lg_w,
    sq_w,
    sk_w,
    sv_w,
    gd_w,
    gu_w,
    dbias,
    head_gain,
    kbias,
    ol_w,
    os_w,
    out,
    w_s,
    gd_s,
    gu_s,
    db_s,
    wol,
    wos,
    tok,
    acc,
    acc_low,
    squares,
    lin_b,
    dlog,
    qx,
    kv,
    bias_s,
    tri,
    o_acc,
    cons,
    far_o,
    far_c,
    far_out,
    ret,
    fin,
    local,
    qstart,
    st_buf,
    td_buf,
    lin_o,
    stk_o,
    lin_r,
    stk_r,
    wsem,
    tok_send,
    tok_recv,
    q_send,
    q_recv,
    ret_send,
    ret_recv,
    bias_send,
    bias_recv,
    kv_send,
    kv_recv,
    st_send,
    st_recv,
    td_send,
    td_recv,
    al_send,
    al_recv,
    as_send,
    as_recv,
):
    me = lax.axis_index("tp")
    here = lax.axis_index("sp")
    T, F = tokens.shape
    H = T // 2
    DK = lq_w.shape[1]
    D = lq_w.shape[0]
    rows_out = T // n_tp
    scale = DK ** (-0.5)
    balanced = n_sp == 4
    reach = 2 if balanced else n_sp

    copies = []
    for i, w in enumerate((sk_w, sv_w, sq_w, lq_w, lk_w, lv_w, lg_w)):
        copies.append(pltpu.make_async_copy(w, w_s.at[:, pl.ds(i * DK, DK)], wsem.at[i]))
    copies.append(pltpu.make_async_copy(gd_w, gd_s, wsem.at[7]))
    col = pl.multiple_of(me * DK, DK)
    copies.append(pltpu.make_async_copy(gu_w.at[:, pl.ds(col, DK)], gu_s, wsem.at[8]))
    copies.append(pltpu.make_async_copy(dbias, db_s, wsem.at[9]))
    copies.append(pltpu.make_async_copy(ol_w, wol, wsem.at[10]))
    copies.append(pltpu.make_async_copy(os_w, wos, wsem.at[11]))
    for c in copies:
        c.start()

    barrier = pltpu.get_barrier_semaphore()
    for d in range(1, n_tp):
        pl.semaphore_signal(
            barrier, inc=1, device_id={"tp": (me + d) % n_tp}, device_id_type=pl.DeviceIdType.MESH
        )
    for d in range(1, n_sp):
        pl.semaphore_signal(
            barrier, inc=1, device_id={"sp": (here + d) % n_sp}, device_id_type=pl.DeviceIdType.MESH
        )
    pl.semaphore_wait(barrier, n_tp + n_sp - 2)

    def remote(src, dst, send, recv, where):
        return pltpu.make_async_remote_copy(
            src_ref=src,
            dst_ref=dst,
            send_sem=send,
            recv_sem=recv,
            device_id=where,
            device_id_type=pl.DeviceIdType.MESH,
        )

    core = me % 2
    chip = me // 2
    side = 1 - 2 * core
    partner = me + side
    x_chip = chip + 1 - 2 * (chip % 2)
    y_step = 2 * (1 - 2 * (chip // 2))
    y_chip = chip + y_step
    d_chip = x_chip + y_step
    x_dev, y_dev, d_dev = 2 * x_chip + core, 2 * y_chip + core, 2 * d_chip + core

    sent = []

    def piece(ref, h):
        return ref.at[pl.ds(h * H, H)]

    def send_tok(src, h, target, own=False):
        dst = tok.at[src, pl.ds(h * H, H)]
        c = remote(
            piece(tokens, h) if own else dst,
            dst,
            tok_send.at[len(sent)],
            tok_recv.at[src, h],
            {"tp": target},
        )
        c.start()
        sent.append(c)

    def wait_tok(src, h):
        dst = tok.at[src, pl.ds(h * H, H)]
        remote(dst, dst, tok_send.at[0], tok_recv.at[src, h], {"tp": partner}).wait_recv()

    send_tok(me, 0, x_dev, True)
    send_tok(me, 1, y_dev, True)
    send_tok(me, 1, x_dev, True)
    send_tok(me, 0, y_dev, True)
    send_tok(me, 0, partner, True)
    send_tok(me, 1, partner, True)

    bias_s[here] = jnp.broadcast_to(kbias[...].astype(F32), bias_s.shape[1:])

    def later(d, make):
        @pl.when(here + d < n_sp)
        def _():
            make(d)

    def bias_copy(d):
        return remote(
            bias_s.at[here], bias_s.at[here], bias_send.at[d], bias_recv.at[here], {"sp": here + d}
        )

    for d in range(1, reach):
        later(d, lambda d: bias_copy(d).start())

    rr = lax.broadcasted_iota(jnp.int32, (T, T), 0)
    cc = lax.broadcasted_iota(jnp.int32, (T, T), 1)
    tri[...] = jnp.where(rr > cc, 1.0, 0.0).astype(BF16)

    def project(src, ref, first=False):
        at = pl.ds(pl.multiple_of(src * F, F), F)
        raw = ref[...].astype(F32)
        sq = raw * raw
        part = sq[:, :128]
        for i in range(1, F // 128):
            part = part + sq[:, i * 128 : (i + 1) * 128]
        scaled = (raw * gain[at].astype(F32)[None, :]).astype(BF16)
        main = fdot(scaled, w_s[at, :])
        low = gdot(scaled, gd_s[:, at], NT)
        if first:
            squares[...] = part
            acc[...] = main
            acc_low[...] = low
        else:
            squares[...] += part
            acc[...] += main
            acc_low[...] += low

    for i in range(8):
        copies[i].wait()
    project(me, tokens, True)
    wait_tok(partner, 0)
    wait_tok(partner, 1)
    project(partner, tok.at[partner])
    wait_tok(x_dev, 0)
    send_tok(x_dev, 0, y_dev)
    send_tok(x_dev, 0, partner)
    wait_tok(y_dev, 1)
    send_tok(y_dev, 1, x_dev)
    send_tok(y_dev, 1, partner)
    wait_tok(x_dev, 1)
    send_tok(x_dev, 1, partner)
    wait_tok(y_dev, 0)
    send_tok(y_dev, 0, partner)
    project(x_dev, tok.at[x_dev])
    project(y_dev, tok.at[y_dev])
    for p in (x_dev + side, y_dev + side):
        wait_tok(p, 0)
        wait_tok(p, 1)
        project(p, tok.at[p])
    wait_tok(d_dev, 0)
    send_tok(d_dev, 0, partner)
    wait_tok(d_dev, 1)
    send_tok(d_dev, 1, partner)
    project(d_dev, tok.at[d_dev])
    wait_tok(d_dev + side, 0)
    wait_tok(d_dev + side, 1)
    project(d_dev + side, tok.at[d_dev + side])

    inv = lax.rsqrt(jnp.sum(squares[...], axis=1, keepdims=True) / D + norm_eps)

    def proj(i):
        return (acc[:, i * DK : (i + 1) * DK] * inv).astype(BF16)

    kv[here, 0] = proj(0)
    kv[here, 1] = proj(1)

    C = CHUNK

    def kv_copy(j, s):
        return remote(kv.at[j], kv.at[j], kv_send.at[s], kv_recv.at[j], {"sp": here + 1})

    split = 0
    parts = ((split, T), (0, split)) if split else ((0, T),)

    def kv_part(j, i):
        lo, hi = parts[i]
        view = kv.at[j, :, pl.ds(lo, hi - lo)]
        return remote(view, view, kv_send.at[i], kv_recv.at[i], {"sp": here + 1})

    @pl.when(here + 1 < n_sp)
    def _():
        if balanced:
            for i in range(len(parts)):
                kv_part(here, i).start()
        else:
            kv_copy(here, 0).start()

    qx[0] = proj(2)

    def q_copy(slot):
        return remote(qx.at[0], qx.at[slot], q_send.at[slot], q_recv.at[slot], {"sp": 2 - slot})

    def ret_copy(i, r, target):
        at = pl.ds(r * C, C)
        return remote(
            far_out.at[i, at], ret.at[at], ret_send.at[i, r], ret_recv.at[r], {"sp": target}
        )

    if balanced:

        @pl.when(here == 3)
        def _():
            q_copy(1).start()

        @pl.when(here == 2)
        def _():
            q_copy(2).start()

    for i in range(4):
        lin_b[i] = proj(3 + i)
    for i in range(8, 10):
        copies[i].wait()
    low = (acc_low[...] * inv).astype(BF16)
    pre = fdot(low, gu_s[...]) + db_s[...]
    dlog[...] = (
        jnp.minimum(pre, 0.0) - jnp.log(1.0 + jnp.exp(-jnp.abs(pre)))
    ) / gate_softness

    row = lax.broadcasted_iota(jnp.int32, (C, DK), 0)
    rc = lax.broadcasted_iota(jnp.int32, (C, C), 0)
    ccol = lax.broadcasted_iota(jnp.int32, (C, C), 1)
    tri_c = jnp.where(rc >= ccol, 1.0, 0.0).astype(F32)

    def chunk(n, carry):
        state, offset = carry
        at = pl.ds(pl.multiple_of(n * C, C), C)
        lam = dlog[at, :]
        c = jnp.dot(tri_c, lam, preferred_element_type=F32, precision=lax.Precision.HIGHEST)
        q = lin_b[0, at, :].astype(F32) * scale
        k = lin_b[1, at, :].astype(F32)
        v = lin_b[2, at, :]
        v32 = v.astype(F32)
        scores = jnp.zeros((C, C), F32)
        m = C // 2
        while m >= 8:
            grouped = c.reshape(C // (2 * m), 2 * m, DK)
            middle = jnp.broadcast_to(grouped[:, m - 1 : m, :], grouped.shape).reshape(C, DK)
            upper = row % (2 * m) >= m
            a = jnp.where(upper, q, k) * jnp.exp(jnp.where(upper, c - middle, middle - c))
            ab = a.astype(BF16)
            pair = gdot(ab, ab, NT)
            keep = (
                (rc // (2 * m) == ccol // (2 * m))
                & (rc % (2 * m) >= m)
                & (ccol % (2 * m) < m)
            )
            scores = jnp.where(keep, pair, scores)
            m //= 2
        total = fdot(scores.astype(BF16), v)
        for delta in range(8):
            if delta == 0:
                p = jnp.sum(q * k, axis=1, keepdims=True)
                total = total + p * v32
                continue
            kd = pltpu.roll(k, delta, 0)
            cd = pltpu.roll(c, delta, 0)
            vd = pltpu.roll(v32, delta, 0)
            p = jnp.sum(q * kd * jnp.exp(jnp.minimum(c - cd, 0.0)), axis=1, keepdims=True)
            total = total + jnp.where(row % 8 >= delta, p * vd, 0.0)
        total = total + gdot((q * jnp.exp(c)).astype(BF16), state.astype(BF16), NT)
        local[at, :] = total
        qstart[at, :] = (q * jnp.exp(offset + c)).astype(BF16)
        last = c[C - 1 : C, :]
        kk = (k * jnp.exp(last - c)).astype(BF16)
        state = state * jnp.exp(last) + gdot(v, kk, TN)
        return state, offset + last

    state, offset = lax.fori_loop(
        0, T // C, chunk, (jnp.zeros((DK, DK), F32), jnp.zeros((1, DK), F32))
    )
    st_buf[here] = state.astype(BF16)
    td_buf[here] = jnp.broadcast_to(offset, td_buf.shape[1:])

    def st_copy(d):
        return remote(
            st_buf.at[here], st_buf.at[here], st_send.at[d], st_recv.at[here], {"sp": here + d}
        )

    def td_copy(d):
        return remote(
            td_buf.at[here], td_buf.at[here], td_send.at[d], td_recv.at[here], {"sp": here + d}
        )

    for d in range(n_sp - 1, 0, -1):
        later(d, lambda d: st_copy(d).start())
        later(d, lambda d: td_copy(d).start())

    def stick(slot, j, mode, o_ref, c_ref, keys=(0, T), finish=None):
        own = mode == "own"
        lo = keys[0]
        for r in range(T // C):
            at = pl.ds(r * C, C)
            n = (r + 1) * C if own else keys[1] - lo
            bias = bias_s[j, 0:1, pl.ds(lo, n)]
            z = gdot(qx[slot, at, :], kv[j, 0, pl.ds(lo, n), :], NT) * scale + bias
            soft = jnp.log(1.0 + jnp.exp(-jnp.abs(z)))
            rise = jnp.minimum(z, 0.0) - soft
            fall = jnp.minimum(-z, 0.0) - soft
            if own:
                tr = lax.broadcasted_iota(jnp.int32, (C, n), 0) + r * C
                visible = lax.broadcasted_iota(jnp.int32, (C, n), 1) < tr
                fall = jnp.where(visible, fall, 0.0)
            high = fall.astype(BF16)
            rest = (fall - high.astype(F32)).astype(BF16)
            later_keys = tri[pl.ds(0, n), pl.ds(0, n)]
            behind = fdot(high, later_keys) + fdot(rest, later_keys)
            power = rise + behind
            if mode == "add":
                power = power + c_ref[at, 0:1]
            share = jnp.exp(power)
            if own:
                share = jnp.where(visible, share, 0.0)
            value = fdot(share.astype(BF16), kv[j, 1, pl.ds(lo, n), :])
            spent = jnp.broadcast_to(behind[:, 0:1] + fall[:, 0:1], (C, DK))
            if mode == "add":
                value = value + o_ref[at, :]
                spent = spent + c_ref[at, :]
            if finish is None:
                o_ref[at, :] = value
                c_ref[at, :] = spent
            else:
                finish(r, value)

    stick(0, here, "own", o_acc, cons)

    def await_kv(j, s):
        remote(kv.at[j], kv.at[j], kv_send.at[s], kv_recv.at[j], {"sp": here}).wait_recv()

    def await_bias(j):
        remote(
            bias_s.at[j], bias_s.at[j], bias_send.at[0], bias_recv.at[j], {"sp": here}
        ).wait_recv()

    def take(s):
        j = here - s
        await_kv(j, s)

        @pl.when(here + 1 < n_sp)
        def _():
            kv_copy(j, s).start()

        await_bias(j)
        stick(0, j, "add", o_acc, cons)

    def give(i, target):
        def finish(r, value):
            far_out[i, pl.ds(r * C, C), :] = value.astype(BF16)
            ret_copy(i, r, target).start()

        return finish

    if balanced:
        last = len(parts) - 1

        @pl.when(here == 1)
        def _():
            q_copy(1).wait_recv()
            stick(1, 1, "start", far_o, far_c)
            await_bias(0)
            for i in range(len(parts)):
                kv_part(0, i).wait_recv()
                stick(1, 0, "add", far_o, far_c, parts[i], give(0, 3) if i == last else None)

        @pl.when(here == 0)
        def _():
            q_copy(2).wait_recv()
            stick(2, 0, "start", far_o, far_c, finish=give(1, 2))

        @pl.when(here >= 2)
        def _():
            await_bias(here - 1)
            for i in range(len(parts)):
                kv_part(here - 1, i).wait_recv()
            stick(0, here - 1, "add", o_acc, cons)

    else:

        @pl.when(here >= 1)
        def _():
            take(1)

    def gather_state(j, incoming):
        remote(st_buf.at[j], st_buf.at[j], st_send.at[0], st_recv.at[j], {"sp": here}).wait_recv()
        remote(td_buf.at[j], td_buf.at[j], td_send.at[0], td_recv.at[j], {"sp": here}).wait_recv()
        return incoming * jnp.exp(td_buf[j][0:1, :]) + st_buf[j].astype(F32)

    incoming = lax.fori_loop(0, here, gather_state, jnp.zeros((DK, DK), F32))
    combined = local[...] + gdot(qstart[...], incoming.astype(BF16), NT)
    normed = (
        combined
        * lax.rsqrt(jnp.mean(combined * combined, axis=1, keepdims=True) + norm_eps)
        * head_gain[...]
    )
    gate = lin_b[3].astype(F32)
    lin_o[...] = (normed * (gate / (1.0 + jnp.exp(-gate)))).astype(BF16)

    def exchange(source, landing, send, recv):
        done = []
        for d in range(1, n_tp):
            p = (me + d) % n_tp
            c = remote(
                source.at[pl.ds(pl.multiple_of(p * rows_out, rows_out), rows_out)],
                landing.at[me],
                send.at[d],
                recv.at[me],
                {"tp": p},
            )
            c.start()
            done.append(c)
        own = pl.ds(pl.multiple_of(me * rows_out, rows_out), rows_out)
        landing[me] = source[own, :]
        return done

    def arrive(landing, recv):
        for d in range(1, n_tp):
            p = (me + d) % n_tp
            remote(landing.at[p], landing.at[p], recv.at[p], recv.at[p], {"tp": p}).wait_recv()

    lin_sent = exchange(lin_o, lin_r, al_send, al_recv)

    if balanced:

        @pl.when(here == 1)
        def _():
            stick(0, 0, "add", o_acc, cons)

        @pl.when(here >= 2)
        def _():
            for r in range(T // C):
                ret_copy(0, r, here).wait_recv()
            o_acc[...] += jnp.exp(cons[...]) * ret[...].astype(F32)

    else:

        def more(s, carry):
            take(s)
            return carry

        lax.fori_loop(2, here + 1, more, 0)

    stk_o[...] = o_acc[...].astype(BF16)
    stk_sent = exchange(stk_o, stk_r, as_send, as_recv)
    copies[10].wait()
    copies[11].wait()
    arrive(lin_r, al_recv)

    def gathered(landing):
        return jnp.concatenate([landing[p] for p in range(n_tp)], axis=1)

    fin[...] = fdot(gathered(lin_r), wol[...])
    arrive(stk_r, as_recv)
    out[...] = (fin[...] + fdot(gathered(stk_r), wos[...])).astype(BF16)

    for c in sent + lin_sent + stk_sent:
        c.wait_send()
    for d in range(1, reach):
        later(d, lambda d: bias_copy(d).wait_send())
    for d in range(1, n_sp):
        later(d, lambda d: st_copy(d).wait_send())
        later(d, lambda d: td_copy(d).wait_send())

    @pl.when(here + 1 < n_sp)
    def _():
        if balanced:
            for i in range(len(parts)):
                kv_part(here, i).wait_send()
        else:

            def drain(s, carry):
                kv_copy(here - s, s).wait_send()
                return carry

            lax.fori_loop(0, here + 1, drain, 0)

    if balanced:

        @pl.when(here == 3)
        def _():
            q_copy(1).wait_send()

        @pl.when(here == 2)
        def _():
            q_copy(2).wait_send()

        @pl.when(here == 1)
        def _():
            for r in range(T // C):
                ret_copy(0, r, 3).wait_send()

        @pl.when(here == 0)
        def _():
            for r in range(T // C):
                ret_copy(1, r, 2).wait_send()


def pipelined(
    n_sp,
    n_tp,
    tokens,
    gain,
    lq_w,
    lk_w,
    lv_w,
    lg_w,
    sq_w,
    sk_w,
    sv_w,
    gd_w,
    gu_w,
    dbias,
    head_gain,
    kbias,
    ol_w,
    os_w,
    out,
    gain_s,
    hg_s,
    kb_s,
    w_s,
    gd_s,
    gu_s,
    db_s,
    wol,
    wos,
    tok,
    acc,
    squares,
    lin_b,
    lams,
    cums,
    qe,
    qstart,
    snap,
    state_s,
    offset_s,
    qx,
    kv,
    bias_s,
    tri,
    o_acc,
    cons,
    near,
    decay,
    far,
    local,
    st_buf,
    lin_o,
    lin_r,
    near_r,
    decay_r,
    far_r,
    fin,
    wsem,
    tok_send,
    tok_recv,
    q_send,
    q_recv,
    bias_send,
    bias_recv,
    kv_send,
    kv_recv,
    st_send,
    st_recv,
    al_send,
    al_recv,
    an_send,
    an_recv,
    ad_send,
    ad_recv,
    af_send,
    af_recv,
):
    me = lax.axis_index("tp")
    here = lax.axis_index("sp")
    T, F = tokens.shape
    C = CHUNK
    HALF = C // 2
    NC = T // C
    DK = lq_w.shape[1]
    D = lq_w.shape[0]
    rank = gd_w.shape[0]
    rows_out = T // n_tp
    scale = DK ** (-0.5)

    barrier = pltpu.get_barrier_semaphore()
    for d in range(1, n_tp):
        pl.semaphore_signal(
            barrier, inc=1, device_id={"tp": (me + d) % n_tp}, device_id_type=pl.DeviceIdType.MESH
        )
    for d in range(1, n_sp):
        pl.semaphore_signal(
            barrier, inc=1, device_id={"sp": (here + d) % n_sp}, device_id_type=pl.DeviceIdType.MESH
        )

    copies = [pltpu.make_async_copy(tokens, tok.at[me], wsem.at[12])]
    copies.append(pltpu.make_async_copy(gain, gain_s, wsem.at[13]))
    copies.append(pltpu.make_async_copy(kbias, kb_s, wsem.at[14]))
    for i, w in enumerate((sk_w, sv_w, sq_w, lq_w, lk_w, lv_w, lg_w)):
        copies.append(pltpu.make_async_copy(w, w_s.at[:, pl.ds(i * DK, DK)], wsem.at[i]))
    copies.append(pltpu.make_async_copy(gd_w, gd_s, wsem.at[7]))
    col = pl.multiple_of(me * DK, DK)
    late = [pltpu.make_async_copy(gu_w.at[:, pl.ds(col, DK)], gu_s, wsem.at[8])]
    late.append(pltpu.make_async_copy(dbias, db_s, wsem.at[9]))
    late.append(pltpu.make_async_copy(head_gain, hg_s, wsem.at[15]))
    wide = [pltpu.make_async_copy(ol_w, wol, wsem.at[10])]
    wide.append(pltpu.make_async_copy(os_w, wos, wsem.at[11]))
    for c in copies + late:
        c.start()

    def remote(src, dst, send, recv, where):
        return pltpu.make_async_remote_copy(
            src_ref=src,
            dst_ref=dst,
            send_sem=send,
            recv_sem=recv,
            device_id=where,
            device_id_type=pl.DeviceIdType.MESH,
        )

    core = me % 2
    chip = me // 2
    side = 1 - 2 * core
    partner = me + side
    x_chip = chip + 1 - 2 * (chip % 2)
    y_step = 2 * (1 - 2 * (chip // 2))
    y_chip = chip + y_step
    d_chip = x_chip + y_step
    x_dev, y_dev, d_dev = 2 * x_chip + core, 2 * y_chip + core, 2 * d_chip + core

    sent = []

    def tok_at(src, i, n):
        return tok.at[src, pl.ds(i * HALF, n * HALF)]

    def send_tok(src, i, n, target):
        at = tok_at(src, i, n)
        c = remote(at, at, tok_send.at[len(sent)], tok_recv.at[src, i], {"tp": target})
        c.start()
        sent.append(c)

    def wait_tok(src, i, n=1):
        at = tok_at(src, i, n)
        remote(at, at, tok_send.at[0], tok_recv.at[src, i], {"tp": partner}).wait_recv()

    def own(i):
        send_tok(me, i, 1, x_dev)
        send_tok(me, i ^ 1, 1, y_dev)

    copies[0].wait()
    pl.semaphore_wait(barrier, n_tp + n_sp - 2)
    own(0)
    own(1)
    for c in range(1, NC):
        own(2 * c)
    for c in range(NC):
        send_tok(me, 2 * c, 2, partner)

    copies[1].wait()
    copies[2].wait()
    bias_s[0] = jnp.broadcast_to(kb_s[...].astype(F32) * LOG2E, bias_s.shape[1:])

    def later(d, make):
        @pl.when(here + d < n_sp)
        def _():
            make(d)

    def bias_copy():
        return remote(
            bias_s.at[0], bias_s.at[1], bias_send.at[0], bias_recv.at[0], {"sp": here + 1}
        )

    later(1, lambda d: bias_copy().start())

    rr = lax.broadcasted_iota(jnp.int32, (2 * C, 2 * C), 0)
    cc = lax.broadcasted_iota(jnp.int32, (2 * C, 2 * C), 1)
    tri[...] = jnp.where((rr % C >= cc) | (cc >= C), 1.0, 0.0).astype(BF16)

    for c in copies[3:]:
        c.wait()
    for c in wide:
        c.start()
    pick = jnp.where(
        lax.broadcasted_iota(jnp.int32, (rank, DK), 0)
        == lax.broadcasted_iota(jnp.int32, (rank, DK), 1),
        1.0,
        0.0,
    ).astype(BF16)
    w_s[:, pl.ds(7 * DK, DK)] = gdot(gd_s[...], pick, TN).astype(BF16)

    def scaled(src, c):
        at = pl.ds(pl.multiple_of(src * F, F), F)
        raw = tok[src, pl.ds(c * C, C), :].astype(F32)
        sq = raw * raw
        part = sq[:, :128]
        for i in range(1, F // 128):
            part = part + sq[:, i * 128 : (i + 1) * 128]
        return (raw * gain_s[at].astype(F32)[None, :]).astype(BF16), part, at

    def group(c, srcs, first=False):
        rows = pl.ds(c * C, C)
        terms = [scaled(s, c) for s in srcs]
        part = terms[0][1] + terms[1][1]
        main = fdot(terms[0][0], w_s[terms[0][2], :]) + fdot(terms[1][0], w_s[terms[1][2], :])
        if first:
            squares[rows, :] = part
            acc[rows, :] = main
        else:
            squares[rows, :] += part
            acc[rows, :] += main

    def kv_copy(c):
        rows = pl.ds(c * C, C)
        return remote(
            kv.at[0, :, rows], kv.at[1, :, rows], kv_send.at[c], kv_recv.at[c], {"sp": here + 1}
        )

    def q_copy(c):
        rows = pl.ds(c * C, C)
        return remote(qx.at[0, rows], qx.at[1, rows], q_send.at[c], q_recv.at[c], {"sp": here - 2})

    def finish(c, srcs):
        rows = pl.ds(c * C, C)
        terms = [scaled(s, c) for s in srcs]
        square = squares[rows, :] + terms[0][1] + terms[1][1]
        inv = lax.rsqrt(jnp.sum(square, axis=1, keepdims=True) / D + norm_eps)

        def columns(h):
            at = pl.ds(h * 4 * DK, 4 * DK)
            total = acc[rows, at]
            for x, _, w_at in terms:
                total = total + fdot(x, w_s[w_at, at])
            return (total * inv).astype(BF16)

        head = columns(0)
        kv[0, 0, rows, :] = head[:, :DK]
        kv[0, 1, rows, :] = head[:, DK : 2 * DK]
        qx[0, rows, :] = head[:, 2 * DK : 3 * DK]
        later(1, lambda d: kv_copy(c).start())

        @pl.when(here >= 2)
        def _():
            q_copy(c).start()

        tail = columns(1)
        lin_b[0, rows, :] = head[:, 3 * DK :]
        for i in range(3):
            lin_b[1 + i, rows, :] = tail[:, i * DK : (i + 1) * DK]
        pre = fdot(tail[:, 3 * DK : 3 * DK + rank], gu_s[...]) + db_s[rows, :]
        lams[rows, :] = (
            jnp.minimum(pre, 0.0) - jnp.log(1.0 + jnp.exp(-jnp.abs(pre)))
        ) / gate_softness

    xs, ys, ds = x_dev + side, y_dev + side, d_dev + side

    for c in range(NC):
        wait_tok(partner, 2 * c, 2)
        group(c, (me, partner), True)

    def turn(c):
        wait_tok(x_dev, 2 * c)
        send_tok(x_dev, 2 * c, 1, y_dev)
        wait_tok(y_dev, 2 * c + 1)
        send_tok(y_dev, 2 * c + 1, 1, x_dev)
        if c + 1 < NC:
            own(2 * c + 3)

    def share_chip(c):
        wait_tok(x_dev, 2 * c + 1)
        send_tok(x_dev, 2 * c, 2, partner)
        wait_tok(y_dev, 2 * c)
        send_tok(y_dev, 2 * c, 2, partner)

    def share_far(c):
        wait_tok(d_dev, 2 * c)
        send_tok(d_dev, 2 * c, 1, partner)
        wait_tok(d_dev, 2 * c + 1)
        send_tok(d_dev, 2 * c + 1, 1, partner)

    def side_chips(c):
        wait_tok(xs, 2 * c, 2)
        wait_tok(ys, 2 * c, 2)
        group(c, (xs, ys))

    def last_chip(c):
        wait_tok(ds, 2 * c)
        wait_tok(ds, 2 * c + 1)
        finish(c, (d_dev, ds))

    row = lax.broadcasted_iota(jnp.int32, (C, DK), 0)
    rc = lax.broadcasted_iota(jnp.int32, (C, C), 0)
    ccol = lax.broadcasted_iota(jnp.int32, (C, C), 1)

    def advance(c):
        rows = pl.ds(c * C, C)
        lam = lams[rows, :]
        high = lam.astype(BF16)
        rest = lam - high.astype(F32)
        mid = rest.astype(BF16)
        low = (rest - mid.astype(F32)).astype(BF16)
        lower = jnp.where(rc >= ccol, 1.0, 0.0).astype(BF16)
        cum = fdot(jnp.concatenate([lower, lower], axis=1), jnp.concatenate([high, mid], axis=0))
        cum = cum + fdot(lower, low)
        cums[rows, :] = cum
        q = lin_b[0, rows, :].astype(F32) * scale
        k = lin_b[1, rows, :].astype(F32)
        v = lin_b[2, rows, :]
        qe[rows, :] = (q * jnp.exp(cum)).astype(BF16)
        last = cum[C - 1 : C, :]
        kk = (k * jnp.exp(last - cum)).astype(BF16)
        fresh = gdot(v, kk, TN)
        if c == 0:
            qstart[rows, :] = (q * jnp.exp(cum)).astype(BF16)
            state_s[...] = fresh
            offset_s[...] = jnp.broadcast_to(last, offset_s.shape)
        else:
            offset = offset_s[0:1, :]
            qstart[rows, :] = (q * jnp.exp(offset + cum)).astype(BF16)
            snap[c] = state_s[...].astype(BF16)
            state_s[...] = state_s[...] * jnp.exp(last) + fresh
            offset_s[...] = jnp.broadcast_to(offset + last, offset_s.shape)

    turn(0)
    share_chip(0)
    group(0, (x_dev, y_dev))
    turn(1)
    turn(2)
    share_far(0)
    side_chips(0)
    share_chip(1)
    for c in late:
        c.wait()
    last_chip(0)
    group(1, (x_dev, y_dev))
    share_far(1)
    share_chip(2)
    side_chips(1)
    last_chip(1)
    group(2, (x_dev, y_dev))
    share_far(2)
    advance(0)
    side_chips(2)
    last_chip(2)
    advance(1)
    advance(2)

    st_buf[here, pl.ds(0, DK), :] = state_s[...].astype(BF16)
    gone = jnp.exp(offset_s[...])
    gone_high = gone.astype(BF16)
    gone_low = (gone - gone_high.astype(F32)).astype(BF16)
    st_buf[here, pl.ds(DK, 16), :] = jnp.concatenate([gone_high, gone_low], axis=0)

    def st_copy(d):
        return remote(
            st_buf.at[here], st_buf.at[here], st_send.at[d], st_recv.at[here], {"sp": here + d}
        )

    for d in range(n_sp - 1, 0, -1):
        later(d, lambda d: st_copy(d).start())

    def within(c):
        rows = pl.ds(c * C, C)
        cum = cums[rows, :]
        lam = lams[rows, :]
        qb = lin_b[0, rows, :]
        kb = lin_b[1, rows, :]
        v = lin_b[2, rows, :]
        q = qb.astype(F32) * scale
        k = kb.astype(F32)
        apart = rc ^ ccol
        scores = gdot(qb, kb, NT) * scale
        m = 1
        while m < C:
            upper = row % (2 * m) >= m
            if m == 1:
                gap = jnp.where(upper, lam, 0.0)
            elif m == 2:
                at = row % 4
                before = pltpu.roll(lam, 1, 0)
                after = pltpu.roll(lam, C - 1, 0)
                gap = jnp.where(upper, jnp.where(at == 3, lam + before, lam), 0.0)
                gap = jnp.where(at == 0, after, gap)
            else:
                grouped = cum.reshape(C // (2 * m), 2 * m, DK)
                middle = jnp.broadcast_to(grouped[:, m - 1 : m, :], grouped.shape).reshape(C, DK)
                gap = jnp.where(upper, cum - middle, middle - cum)
            a = (jnp.where(upper, q, k) * jnp.exp(gap)).astype(BF16)
            scores = jnp.where(apart >= m, gdot(a, a, NT), scores)
            m *= 2
        scores = jnp.where(rc >= ccol, scores, 0.0).astype(BF16)
        total = fdot(scores, v)
        if c:
            total = total + gdot(qe[rows, :], snap[c], NT)
        local[rows, :] = total

    def stick(q, slot, nb, diagonal, run):
        n = nb * C
        z = gdot(q, kv[slot, 0, pl.ds(0, n), :], NT) * (scale * LOG2E) + bias_s[
            slot, 0:1, pl.ds(0, n)
        ]
        loss = jnp.maximum(z, 0.0) + jnp.log(1.0 + jnp.exp2(-jnp.abs(z))) * LOG2E
        shares = []
        for b in reversed(range(nb)):
            at = slice(b * C, (b + 1) * C)
            piece = loss[:, at]
            masked = diagonal and b == nb - 1
            if masked:
                piece = jnp.where(ccol < rc, piece, 0.0)
            high = piece.astype(BF16)
            rest = (piece - high.astype(F32)).astype(BF16)
            sums = fdot(jnp.concatenate([high, rest], axis=1), tri[...])
            power = z[:, at] - sums[:, :C]
            if run is not None:
                power = power - run
            share = jnp.exp2(power)
            if masked:
                share = jnp.where(ccol < rc, share, 0.0)
            shares.append(share.astype(BF16))
            run = sums[:, C:] if run is None else run + sums[:, C:]
        shares = jnp.concatenate(shares[::-1], axis=1) if nb > 1 else shares[0]
        return fdot(shares, kv[slot, 1, pl.ds(0, n), :]), run

    for c in range(NC):
        within(c)
    for r in range(NC):
        rows = pl.ds(r * C, C)
        o_acc[rows, :], cons[rows, :] = stick(qx[0, rows, :], 0, r + 1, True, None)

    def await_kv():
        remote(
            bias_s.at[1], bias_s.at[1], bias_send.at[0], bias_recv.at[0], {"sp": here}
        ).wait_recv()
        for c in range(NC):
            rows = pl.ds(c * C, C)
            at = kv.at[1, :, rows]
            remote(at, at, kv_send.at[c], kv_recv.at[c], {"sp": here}).wait_recv()

    def await_q(r):
        at = qx.at[1, pl.ds(r * C, C)]
        remote(at, at, q_send.at[r], q_recv.at[r], {"sp": here}).wait_recv()

    def far_copy(p):
        return remote(
            far.at[pl.ds(p * rows_out, rows_out)],
            far_r.at[me],
            af_send.at[p],
            af_recv.at[me],
            {"sp": here + 2, "tp": p},
        )

    def give(r, value):
        far[pl.ds(r * C, C), :] = value.astype(BF16)
        for p in range(n_tp):
            if r * C < (p + 1) * rows_out <= (r + 1) * C:
                far_copy(p).start()

    @pl.when(here == 0)
    def _():
        for r in range(NC):
            await_q(r)
            give(r, stick(qx[1, pl.ds(r * C, C), :], 0, NC, False, None)[0])

    @pl.when(here == 1)
    def _():
        await_kv()
        for r in range(NC):
            await_q(r)
            q = qx[1, pl.ds(r * C, C), :]
            nearer, run = stick(q, 0, NC, False, None)
            give(r, nearer + stick(q, 1, NC, False, run)[0])

    @pl.when(here >= 2)
    def _():
        await_kv()

    def exchange(source, landing, send, recv):
        for d in range(1, n_tp):
            p = (me + d) % n_tp
            exchange_copy(source, landing, send, recv, d, p).start()
        mine = pl.ds(pl.multiple_of(me * rows_out, rows_out), rows_out)
        landing[me] = source[mine, :]

    def exchange_copy(source, landing, send, recv, d, p):
        return remote(
            source.at[pl.ds(pl.multiple_of(p * rows_out, rows_out), rows_out)],
            landing.at[me],
            send.at[d],
            recv.at[me],
            {"tp": p},
        )

    def exchanged(source, landing, send, recv):
        for d in range(1, n_tp):
            exchange_copy(source, landing, send, recv, d, (me + d) % n_tp).wait_send()

    @pl.when(here >= 1)
    def _():
        for r in range(NC):
            rows = pl.ds(r * C, C)
            value, run = stick(qx[0, rows, :], 1, NC, False, cons[rows, :])
            o_acc[rows, :] += value
            cons[rows, :] = run

    near[...] = o_acc[...].astype(BF16)
    exchange(near, near_r, an_send, an_recv)

    @pl.when(here >= 2)
    def _():
        decay[...] = jnp.exp2(-cons[...]).astype(BF16)
        exchange(decay, decay_r, ad_send, ad_recv)

    def gather_state(j, incoming):
        remote(st_buf.at[j], st_buf.at[j], st_send.at[0], st_recv.at[j], {"sp": here}).wait_recv()
        shrink = st_buf[j, pl.ds(DK, 16), :].astype(F32)
        kept = shrink[0:1, :] + shrink[8:9, :]
        return incoming * kept + st_buf[j, pl.ds(0, DK), :].astype(F32)

    incoming = lax.fori_loop(0, here, gather_state, jnp.zeros((DK, DK), F32))
    combined = local[...] + gdot(qstart[...], incoming.astype(BF16), NT)
    normed = (
        combined
        * lax.rsqrt(jnp.mean(combined * combined, axis=1, keepdims=True) + norm_eps)
        * hg_s[...]
    )
    gate = lin_b[3].astype(F32)
    lin_o[...] = (normed * (gate / (1.0 + jnp.exp(-gate)))).astype(BF16)
    exchange(lin_o, lin_r, al_send, al_recv)

    for c in wide:
        c.wait()

    chips = (chip, x_chip, y_chip, d_chip)

    def arrive(landing, recv, p):
        remote(landing.at[p], landing.at[p], recv.at[p], recv.at[p], {"tp": p}).wait_recv()

    def product(pair, weight, j, first):
        at = pl.ds(pl.multiple_of(j * 2 * DK, 2 * DK), 2 * DK)
        term = fdot(pair, weight[at, :])
        if first:
            fin[...] = term
        else:
            fin[...] += term

    def pair_of(landing, j):
        return jnp.concatenate([landing[2 * j], landing[2 * j + 1]], axis=1)

    for j in chips:
        for p in (2 * j, 2 * j + 1):
            if j is not chip:
                arrive(near_r, an_recv, p)
    arrive(near_r, an_recv, partner)

    @pl.when(here >= 2)
    def _():
        for j in chips:
            for p in (2 * j, 2 * j + 1):
                if j is not chip:
                    arrive(decay_r, ad_recv, p)
        arrive(decay_r, ad_recv, partner)
        for p in range(n_tp):
            arrive(far_r, af_recv, p)
            near_r[p] = (
                near_r[p].astype(F32) + decay_r[p].astype(F32) * far_r[p].astype(F32)
            ).astype(BF16)

    for i, j in enumerate(chips):
        product(pair_of(near_r, j), wos, j, i == 0)
    for i, j in enumerate(chips):
        if i:
            arrive(lin_r, al_recv, 2 * j)
            arrive(lin_r, al_recv, 2 * j + 1)
        else:
            arrive(lin_r, al_recv, partner)
        if i < len(chips) - 1:
            product(pair_of(lin_r, j), wol, j, False)
    at = pl.ds(pl.multiple_of(d_chip * 2 * DK, 2 * DK), 2 * DK)
    out[...] = (fin[...] + fdot(pair_of(lin_r, d_chip), wol[at, :])).astype(BF16)

    for c in sent:
        c.wait_send()
    exchanged(near, near_r, an_send, an_recv)
    exchanged(lin_o, lin_r, al_send, al_recv)

    @pl.when(here >= 2)
    def _():
        exchanged(decay, decay_r, ad_send, ad_recv)
        for c in range(NC):
            q_copy(c).wait_send()

    @pl.when(here < 2)
    def _():
        for p in range(n_tp):
            far_copy(p).wait_send()

    for d in range(1, n_sp):
        later(d, lambda d: st_copy(d).wait_send())

    @pl.when(here + 1 < n_sp)
    def _():
        bias_copy().wait_send()
        for c in range(NC):
            kv_copy(c).wait_send()


def pipelined_call(n_sp, n_tp, args):
    tokens, lq_w, gd_w, out_linear, out_stick = args[0], args[2], args[9], args[14], args[15]
    T, F = tokens.shape
    D, DK = lq_w.shape
    rank = gd_w.shape[0]
    rows_out = T // n_tp
    width = out_linear.shape[1]
    chunks = T // CHUNK
    dma = pltpu.SemaphoreType.DMA
    landing = pltpu.VMEM((n_tp, rows_out, DK), BF16)
    wide32, wide16 = pltpu.VMEM((T, DK), F32), pltpu.VMEM((T, DK), BF16)
    return pl.pallas_call(
        functools.partial(pipelined, n_sp, n_tp),
        out_shape=pltpu.VMEM((rows_out, width), BF16),
        in_specs=[pl.BlockSpec(memory_space=pl.ANY)] * len(args),
        out_specs=pl.BlockSpec(memory_space=pltpu.VMEM),
        scratch_shapes=[
            pltpu.VMEM((D,), BF16),
            pltpu.VMEM((1, DK), F32),
            pltpu.VMEM((1, T), BF16),
            pltpu.VMEM((D, 8 * DK), BF16),
            pltpu.VMEM((rank, D), BF16),
            pltpu.VMEM((rank, DK), BF16),
            wide32,
            pltpu.VMEM(out_linear.shape, BF16),
            pltpu.VMEM(out_stick.shape, BF16),
            pltpu.VMEM((n_tp, T, F), BF16),
            pltpu.VMEM((T, 8 * DK), F32),
            pltpu.VMEM((T, 128), F32),
            pltpu.VMEM((4, T, DK), BF16),
            wide32,
            wide32,
            wide16,
            wide16,
            pltpu.VMEM((chunks, DK, DK), BF16),
            pltpu.VMEM((DK, DK), F32),
            pltpu.VMEM((8, DK), F32),
            pltpu.VMEM((2, T, DK), BF16),
            pltpu.VMEM((2, 2, T, DK), BF16),
            pltpu.VMEM((2, 8, T), F32),
            pltpu.VMEM((2 * CHUNK, 2 * CHUNK), BF16),
            wide32,
            wide32,
            wide16,
            wide16,
            wide16,
            wide32,
            pltpu.VMEM((n_sp, DK + 16, DK), BF16),
            wide16,
            landing,
            landing,
            landing,
            landing,
            pltpu.VMEM((rows_out, width), F32),
            dma((16,)),
            dma((11 * chunks,)),
            dma((n_tp, 2 * chunks)),
            dma((chunks,)),
            dma((chunks,)),
            dma((1,)),
            dma((1,)),
            dma((chunks,)),
            dma((chunks,)),
            dma((n_sp,)),
            dma((n_sp,)),
        ]
        + [dma((n_tp,))] * 8,
        compiler_params=pltpu.CompilerParams(collective_id=0, has_side_effects=True),
    )(*args)


def per_device(n_sp, n_tp, *args):
    (
        tokens,
        norm_gain,
        lin_query,
        lin_key,
        lin_value,
        lin_gate,
        gate_down,
        gate_up_weight,
        decay_offset_bias,
        lin_norm_gain,
        stick_query,
        stick_key,
        stick_value,
        key_bias,
        out_linear,
        out_stick,
    ) = args
    operands = (
        tokens,
        norm_gain,
        lin_query,
        lin_key,
        lin_value,
        lin_gate,
        stick_query,
        stick_key,
        stick_value,
        gate_down.T,
        gate_up_weight,
        decay_offset_bias,
        lin_norm_gain.reshape(1, -1),
        key_bias,
        out_linear,
        out_stick,
    )
    if n_sp == 4 and n_tp == 8:
        return pipelined_call(n_sp, n_tp, operands)
    T, F = tokens.shape
    D, DK = lin_query.shape
    rank = gate_down.shape[1]
    rows_out = T // n_tp
    width = out_linear.shape[1]
    vm = pl.BlockSpec(memory_space=pltpu.VMEM)
    anywhere = pl.BlockSpec(memory_space=pl.ANY)
    dma = pltpu.SemaphoreType.DMA
    return pl.pallas_call(
        functools.partial(kernel, n_sp, n_tp),
        out_shape=pltpu.VMEM((rows_out, width), BF16),
        in_specs=[vm, vm] + [anywhere] * 10 + [vm, vm, anywhere, anywhere],
        out_specs=vm,
        scratch_shapes=[
            pltpu.VMEM((D, 7 * DK), BF16),
            pltpu.VMEM((rank, D), BF16),
            pltpu.VMEM((rank, DK), BF16),
            pltpu.VMEM((T, DK), F32),
            pltpu.VMEM(out_linear.shape, BF16),
            pltpu.VMEM(out_stick.shape, BF16),
            pltpu.VMEM((n_tp, T, F), BF16),
            pltpu.VMEM((T, 7 * DK), F32),
            pltpu.VMEM((T, rank), F32),
            pltpu.VMEM((T, 128), F32),
            pltpu.VMEM((4, T, DK), BF16),
            pltpu.VMEM((T, DK), F32),
            pltpu.VMEM((3, T, DK), BF16),
            pltpu.VMEM((n_sp, 2, T, DK), BF16),
            pltpu.VMEM((n_sp, 8, T), F32),
            pltpu.VMEM((T, T), BF16),
            pltpu.VMEM((T, DK), F32),
            pltpu.VMEM((T, DK), F32),
            pltpu.VMEM((T, DK), F32),
            pltpu.VMEM((T, DK), F32),
            pltpu.VMEM((2, T, DK), BF16),
            pltpu.VMEM((T, DK), BF16),
            pltpu.VMEM((rows_out, width), F32),
            pltpu.VMEM((T, DK), F32),
            pltpu.VMEM((T, DK), BF16),
            pltpu.VMEM((n_sp, DK, DK), BF16),
            pltpu.VMEM((n_sp, 8, DK), F32),
            pltpu.VMEM((T, DK), BF16),
            pltpu.VMEM((T, DK), BF16),
            pltpu.VMEM((n_tp, rows_out, DK), BF16),
            pltpu.VMEM((n_tp, rows_out, DK), BF16),
            dma((12,)),
            dma((16,)),
            dma((n_tp, 2)),
            dma((3,)),
            dma((3,)),
            dma((2, T // CHUNK)),
            dma((T // CHUNK,)),
            dma((n_sp,)),
            dma((n_sp,)),
            dma((n_sp,)),
            dma((n_sp,)),
            dma((n_sp,)),
            dma((n_sp,)),
            dma((n_sp,)),
            dma((n_sp,)),
            dma((n_tp,)),
            dma((n_tp,)),
            dma((n_tp,)),
            dma((n_tp,)),
        ],
        compiler_params=pltpu.CompilerParams(collective_id=0, has_side_effects=True),
    )(*operands)


def solution(mesh):
    placed = (
        P("sp", "tp"),
        P(),
        P(None, "tp"),
        P(None, "tp"),
        P(None, "tp"),
        P(None, "tp"),
        P(),
        P(),
        P("sp", "tp"),
        P(),
        P(None, "tp"),
        P(None, "tp"),
        P(None, "tp"),
        P("tp", "sp"),
        P(),
        P(),
    )
    return jax.shard_map(
        functools.partial(per_device, mesh.shape["sp"], mesh.shape["tp"]),
        mesh=mesh,
        in_specs=placed,
        out_specs=P(("sp", "tp"), None),
        check_vma=False,
    )
```
